512 devices in a mesh: kv: 32 (over z, core), tp: 16 (over y, x).
Axes of the slice: x: 4, y: 4, z: 16, core: 2. Of those that a mesh axis runs over, the one named last changes fastest.
Arguments:
- tokens: bfloat16 [16, 2048], P(None, 'kv'), may hold values from -8 to 8
- lengths: int32 [16], replicated, may hold values from 1 to 49152, 196608 in all
- latent_cache: bfloat16 [16, 49152, 256], P(None, ('kv', 'tp')), may hold values from -10 to 10
- rope_cache: bfloat16 [16, 49152, 32], P(None, ('kv', 'tp')), may hold values from -2000 to 2000
- gain_in: bfloat16 [2048], P('kv'), may hold values from 0.099609375 to 1.8984375
- w_down_q: bfloat16 [2048, 512], P('kv'), may hold values from -0.125 to 0.125
- w_down_kv: bfloat16 [2048, 256], P('kv'), may hold values from -0.125 to 0.125
- w_rope_key: bfloat16 [2048, 32], P('kv'), may hold values from -0.125 to 0.125
- gain_q: bfloat16 [512], replicated, may hold values from 0.099609375 to 1.8984375
- w_up_qn: bfloat16 [512, 16, 64], replicated, may hold values from -0.25 to 0.25
- w_up_qr: bfloat16 [512, 16, 32], replicated, may hold values from -0.25 to 0.25
- gain_kv: bfloat16 [256], replicated, may hold values from 0.099609375 to 1.8984375
- w_key_up: bfloat16 [256, 16, 64], replicated, may hold values from -0.375 to 0.375
- w_value_up: bfloat16 [256, 16, 64], replicated, may hold values from -0.375 to 0.375
- w_attn_out: bfloat16 [16, 64, 2048], P('tp', None, 'kv'), may hold values from -0.1875 to 0.1875
- gain_mid: bfloat16 [2048], P('kv'), may hold values from 0.099609375 to 1.8984375
- w_ff_in: bfloat16 [2048, 8192], P('kv', 'tp'), may hold values from -0.125 to 0.125
- w_ff_out: bfloat16 [8192, 2048], P('tp', 'kv'), may hold values from -0.0625 to 0.0625
Outputs:
- mixed: bfloat16 [16, 2048], P(None, 'kv')
- new_latent: bfloat16 [16, 256], replicated
- new_rope_key: bfloat16 [16, 32], replicated
The draws below stay inside these ranges and needn't reach their ends.
Inputs may be any that keep to these rules, and one draw needn't show every extreme that they name: `lengths`: each sequence's live cache positions; one sequence fills the whole cache.
All inputs are finite; a program needn't handle non-finite values.
Results may differ from the reference program's by a relative error of at most 0.012.
Values sent between devices are 32-bit elements; how exact they have to be, the bound alone decides.
A program may use at most 64 MiB of HBM per device.

```python
import math
import jax
import jax.numpy as jnp
import numpy as np
from jax import lax

D = 2048
H = 16
NOPE = 64
ROPE = 32
V = 64
QR = 512
KR = 256
FF = 8192
SEQS = 16
CACHE = 49152
N_KV = 32


def draw_tokens(key, part):
    first = jax.random.fold_in(key, 0)
    rising = 0.3 * 10.0 ** (jnp.arange(D, dtype=jnp.float32) / D)
    values = jax.random.normal(first, (SEQS, D), jnp.float32) * rising
    return jnp.clip(values, -8.0, 8.0).astype(jnp.bfloat16)


def draw_latent_cache(key, part):
    first = jax.random.fold_in(key, 0)
    values = jax.random.normal(first, (SEQS, CACHE, KR), jnp.float32) * 2.0
    return jnp.clip(values, -10.0, 10.0).astype(jnp.bfloat16)


def draw_rope_cache(key, part):
    first = jax.random.fold_in(key, 0)
    values = jax.random.normal(first, (SEQS, CACHE, ROPE), jnp.float32) * 2.0
    return jnp.clip(values, -2000.0, 2000.0).astype(jnp.bfloat16)


def levels(own_key, dims, cuts, low, top_value):
    factor_of, own = 1.0, jax.random.fold_in(own_key, 6)
    for dim, shards_of in cuts:
        draws = jnp.exp(jax.random.uniform(jax.random.fold_in(own, dim), (shards_of,), jnp.float32, low / len(cuts), top_value / len(cuts)))
        factor_of = factor_of * jnp.repeat(draws, dims[dim] // shards_of).reshape([-1 if axis == dim else 1 for axis in range(len(dims))])
    return factor_of


def profile(count, total, limit, slope):
    portions = [(1 << 20) // math.isqrt(rank ** slope) + 1 for rank in range(2, count + 1)]
    surplus, holding = total - limit - (count - 1), [1] * (count - 1)
    while surplus > 0:
        movable = [i for i in range(count - 1) if holding[i] < limit]
        whole, left = sum([portions[i] for i in movable]), surplus
        for i in movable:
            more = min(limit - holding[i], max(1, left * portions[i] // whole), surplus)
            holding[i] = holding[i] + more
            surplus = surplus - more
    return np.array([limit] + holding)


def uneven(key, amount, total, most, lean):
    if amount == 2:
        one = jax.random.randint(key, (), max(1, total - most), min(most, total - 1) + 1)
        return jnp.stack([one, total - one])
    sizes = jnp.asarray(profile(amount, total, most, lean), jnp.int32)
    pairs = (amount - 1) // 2
    donor, receiver = sizes[1:1 + 2 * pairs:2], sizes[2:2 + 2 * pairs:2]
    slack = jnp.minimum(donor - 1, most - receiver)
    moved = jax.random.randint(jax.random.fold_in(key, 1), (pairs,), 0, 1 << 20) % (slack + 1)
    sizes = sizes.at[1:1 + 2 * pairs:2].set(donor - moved).at[2:2 + 2 * pairs:2].set(receiver + moved)
    return sizes[jax.random.permutation(jax.random.fold_in(key, 2), amount)]


def scatter_about(rng, extent, deviation, most, cuts=(), kind=jnp.bfloat16):
    level = levels(rng, extent, cuts, -0.22, 0.18) if cuts else 1.0
    drawn = jax.random.normal(rng, extent, jnp.float32) * deviation * level
    return jnp.minimum(jnp.maximum(drawn, -most), most).astype(kind)


def setup_inputs(seed: int = 0) -> dict:
    streams_of = jax.random.split(jax.random.key(seed), 19)
    return {
        "tokens": draw_tokens(jax.random.fold_in(streams_of[18], 71), 0),
        "lengths": uneven(streams_of[1], SEQS, SEQS * CACHE // 4, CACHE, 2).astype(jnp.int32),
        "latent_cache": draw_latent_cache(jax.random.fold_in(streams_of[18], 71), 0),
        "rope_cache": draw_rope_cache(jax.random.fold_in(streams_of[18], 71), 0),
        "gain_in": jnp.clip(1.0 + 0.18 * jax.random.normal(streams_of[4], (D,), jnp.float32), 0.099609375, 1.8984375).astype(jnp.bfloat16),
        "w_down_q": scatter_about(streams_of[5], (D, QR), D ** -0.5, 0.125, ((0, 32),)),
        "w_down_kv": scatter_about(streams_of[6], (D, KR), D ** -0.5, 0.125, ((0, 32),)),
        "w_rope_key": scatter_about(streams_of[7], (D, ROPE), D ** -0.5, 0.125, ((0, 32),)),
        "gain_q": jnp.clip(1.0 + 0.18 * jax.random.normal(streams_of[8], (QR,), jnp.float32), 0.099609375, 1.8984375).astype(jnp.bfloat16),
        "w_up_qn": scatter_about(streams_of[9], (QR, H, NOPE), QR ** -0.5, 0.25),
        "w_up_qr": scatter_about(streams_of[10], (QR, H, ROPE), QR ** -0.5, 0.25),
        "gain_kv": jnp.clip(1.0 + 0.18 * jax.random.normal(streams_of[11], (KR,), jnp.float32), 0.099609375, 1.8984375).astype(jnp.bfloat16),
        "w_key_up": scatter_about(streams_of[12], (KR, H, NOPE), KR ** -0.5, 0.375),
        "w_value_up": scatter_about(streams_of[13], (KR, H, V), KR ** -0.5, 0.375),
        "w_attn_out": scatter_about(streams_of[14], (H, V, D), (H * V) ** -0.5, 0.1875, ((0, 16), (2, 32))),
        "gain_mid": jnp.clip(1.0 + 0.18 * jax.random.normal(streams_of[15], (D,), jnp.float32), 0.099609375, 1.8984375).astype(jnp.bfloat16),
        "w_ff_in": scatter_about(streams_of[16], (D, FF), D ** -0.5, 0.125, ((0, 32), (1, 16))),
        "w_ff_out": scatter_about(streams_of[17], (FF, D), FF ** -0.5, 0.0625, ((0, 16), (1, 32))),
    }


EPS = 1e-06

def rotate(values, positions):
    half = values.shape[-1] // 2
    inverse = 10000.0 ** (-jnp.arange(half, dtype=jnp.float32) / half)
    angle = positions.astype(jnp.float32)[:, None, None] * inverse[None, None, :]
    first = values[..., :half]
    second = values[..., half:]
    return jnp.concatenate([first * jnp.cos(angle) - second * jnp.sin(angle), second * jnp.cos(angle) + first * jnp.sin(angle)], axis=-1)

def rms_scaled(values, gain):
    return values * lax.rsqrt(lax.optimization_barrier(jnp.mean(values * values, axis=-1, keepdims=True)) + EPS) * gain.astype(jnp.float32)

def reference(tokens, lengths, latent_cache, rope_cache, gain_in, w_down_q, w_down_kv, w_rope_key, gain_q, w_up_qn, w_up_qr, gain_kv, w_key_up, w_value_up, w_attn_out, gain_mid, w_ff_in, w_ff_out):
    f32 = jnp.float32
    bf16 = jnp.bfloat16
    scale = (NOPE + ROPE) ** (-0.5)
    resid = tokens.astype(f32)
    scaled_in = (resid * gain_in.astype(f32)).astype(bf16)
    inv_in = lax.rsqrt(lax.optimization_barrier(jnp.mean(resid * resid, axis=1, keepdims=True)) + EPS)
    sum_q = jnp.dot(scaled_in, w_down_q, preferred_element_type=f32)
    sum_kv = jnp.dot(scaled_in, w_down_kv, preferred_element_type=f32)
    sum_rope = jnp.dot(scaled_in, w_rope_key, preferred_element_type=f32)
    query_latent = rms_scaled(inv_in * sum_q, gain_q).astype(bf16)
    new_latent = rms_scaled(inv_in * sum_kv, gain_kv).astype(bf16)
    new_rope_key = rotate((inv_in * sum_rope)[:, None, :], lengths)[:, 0, :].astype(bf16)
    query_nope = jnp.einsum('bc,chd->bhd', query_latent.astype(f32), w_up_qn.astype(f32)).astype(bf16)
    query_rope = rotate(jnp.einsum('bc,chr->bhr', query_latent.astype(f32), w_up_qr.astype(f32)), lengths).astype(bf16)
    query_cache = jnp.einsum('bhd,khd->bhk', query_nope.astype(f32), w_key_up.astype(f32)).astype(bf16)
    self_score = (jnp.einsum('bhk,bk->bh', query_cache.astype(f32), new_latent.astype(f32)) + jnp.einsum('bhr,br->bh', query_rope.astype(f32), new_rope_key.astype(f32))) * scale
    span = CACHE // N_KV
    latent_blocks = latent_cache.reshape(SEQS, N_KV, span, KR).swapaxes(0, 1)
    rope_blocks = rope_cache.reshape(SEQS, N_KV, span, ROPE).swapaxes(0, 1)

    def block_scores(args):
        latent_block, rope_block, index = args
        scores = (jnp.einsum('bhk,blk->bhl', query_cache.astype(f32), latent_block.astype(f32)) + jnp.einsum('bhr,blr->bhl', query_rope.astype(f32), rope_block.astype(f32))) * scale
        positions = index * span + jnp.arange(span, dtype=jnp.int32)
        live = positions[None, :] < lengths[:, None]
        return (jnp.where(live[:, None, :], scores, -1e+30), live)
    scores, lives = lax.map(block_scores, (latent_blocks, rope_blocks, jnp.arange(N_KV, dtype=jnp.int32)))
    top = jnp.maximum(lax.optimization_barrier(jnp.max(scores, axis=(0, 3))), self_score)
    weights = jnp.where(lives[:, :, None, :], jnp.exp(scores - top[None, :, :, None]), 0.0)
    self_weight = jnp.exp(self_score - top)
    total = lax.optimization_barrier(jnp.sum(weights, axis=(0, 3))) + self_weight

    def add_block(acc, args):
        weight_block, latent_block = args
        term = jnp.einsum('bhl,blk->bhk', weight_block.astype(bf16).astype(f32), latent_block.astype(f32))
        return (acc + term, None)
    start = self_weight.astype(bf16).astype(f32)[:, :, None] * new_latent.astype(f32)[:, None, :]
    acc, _ = lax.scan(add_block, start, (weights, latent_blocks))
    expanded = jnp.einsum('bhk,khv->bhv', acc, w_value_up.astype(f32), precision=lax.Precision.HIGHEST)
    head_out = (expanded / total[:, :, None]).astype(bf16)
    resid_mid = resid + jnp.einsum('bhv,hvd->bd', head_out.astype(f32), w_attn_out.astype(f32))
    scaled_mid = (resid_mid * gain_mid.astype(f32)).astype(bf16)
    inv_mid = lax.rsqrt(lax.optimization_barrier(jnp.mean(resid_mid * resid_mid, axis=1, keepdims=True)) + EPS)
    hidden = jnp.square(jax.nn.relu(inv_mid * jnp.dot(scaled_mid, w_ff_in, preferred_element_type=f32))).astype(bf16)
    mixed = (resid_mid + jnp.dot(hidden, w_ff_out, preferred_element_type=f32)).astype(bf16)
    return (mixed, new_latent, new_rope_key)
```

```python
import functools

import jax
import jax.numpy as jnp
import numpy as np
from jax import lax
from jax.experimental import pallas as pl
from jax.experimental.pallas import tpu as pltpu
from jax.sharding import Mesh
from jax.sharding import PartitionSpec as P

D = 2048
H = 16
NOPE = 64
ROPE = 32
NZ = 16
NT = 16
SEQS = 16
SPAN = 96
KR = 256
EPS = 1e-06
SCALE = (NOPE + ROPE) ** (-0.5)
MESH = pl.DeviceIdType.MESH
f32 = jnp.float32
bf16 = jnp.bfloat16

Z_OFFSETS = sorted(range(1, NZ), key=lambda d: -min(d, NZ - d))


def torus_distance(d):
    y, x = d // 4, d % 4
    return min(y, 4 - y) + min(x, 4 - x)


def nt(a, b):
    return lax.dot_general(a, b, (((1,), (1,)), ((), ())), preferred_element_type=f32)


def nn(a, b):
    return jnp.dot(a, b, preferred_element_type=f32)


def rotated(x, cos, sin, low):
    n = x.shape[-1]
    swapped = jnp.where(low, pltpu.roll(x, n - 16, 1), pltpu.roll(x, 16, 1))
    return x * cos + swapped * sin


def merged(pieces, lane):
    tops = [jnp.broadcast_to(p[:, 64:65], p.shape) for p in pieces]
    top = functools.reduce(jnp.maximum, tops)
    out = None
    for p, own in zip(pieces, tops):
        term = p * jnp.exp(own - top)
        out = term if out is None else out + term
    return top, jnp.where(lane == 64, top, out)


def kernel(
    tokens,
    lengths,
    latent,
    rope,
    gain_in,
    w_q,
    w_kv,
    w_rope,
    gain_q,
    w_qn,
    w_qr,
    gain_kv,
    w_k,
    w_v,
    w_ao,
    gain_mid,
    w_in,
    w_out,
    freq,
    mixed,
    new_latent,
    new_rope,
    tokens_s,
    lengths_s,
    latent_s,
    rope_s,
    gain_in_s,
    w_q_s,
    w_kv_s,
    w_rope_s,
    gain_q_s,
    w_qn_s,
    w_qr_s,
    gain_kv_s,
    w_k_s,
    w_v_s,
    w_ao_s,
    gain_mid_s,
    w_in_s,
    w_out_s,
    freq_s,
    part_s,
    pair_a,
    pair_small,
    pair_big,
    a1,
    a2,
    qc_s,
    qr_s,
    acc_s,
    st_s,
    nl_s,
    b_send,
    b_recv,
    c_recv,
    d_recv,
    rm_all,
    e_send,
    e_recv,
    g_recv,
    hid_s,
    f_recv,
    load_sem,
    send_sem,
    recv_sem,
):
    z, c, t = lax.axis_index("z"), lax.axis_index("core"), lax.axis_index("tp")
    other = 1 - c
    barrier = pltpu.get_barrier_semaphore()
    z_peers = [(lax.rem(z + d, NZ), c, t) for d in Z_OFFSETS]
    t_order = sorted(range(1, NT), key=lambda d: -torus_distance(d))
    t_peers = [lax.rem(t // 4 + d // 4, 4) * 4 + lax.rem(lax.rem(t, 4) + d % 4, 4) for d in t_order]
    plane_peers = [(z, k, u) for u in t_peers for k in (c, other)] + [(z, other, t)]
    partner = (z, other, t)
    slot = 2 * t + c

    for peer in z_peers + plane_peers:
        pl.semaphore_signal(barrier, inc=1, device_id=peer, device_id_type=MESH)

    sources = (tokens, gain_in, w_q, w_kv, w_rope, lengths, freq, w_in, w_out, w_ao, gain_mid, gain_q, gain_kv, w_qn, w_qr, w_k, latent, rope, w_v)
    targets = (tokens_s, gain_in_s, w_q_s, w_kv_s, w_rope_s, lengths_s, freq_s, w_in_s, w_out_s, w_ao_s, gain_mid_s, gain_q_s, gain_kv_s, w_qn_s, w_qr_s, w_k_s, latent_s, rope_s, w_v_s)
    loads = [
        pltpu.make_async_copy(source, target, load_sem.at[i])
        for i, (source, target) in enumerate(zip(sources, targets))
    ]
    for load in loads:
        load.start()

    def send(source, target, phase, device):
        pltpu.make_async_remote_copy(
            source, target, send_sem.at[phase], recv_sem.at[phase], device_id=device, device_id_type=MESH
        ).start()

    def arrived(ref, phase):
        pltpu.make_async_copy(ref, ref, recv_sem.at[phase]).wait()

    def sent(ref, phase):
        pltpu.make_async_copy(ref, ref, send_sem.at[phase]).wait()

    lane = lax.broadcasted_iota(jnp.int32, (8, 128), 1)
    lane16 = lax.broadcasted_iota(jnp.int32, (16, 128), 1)

    for load in loads[:5]:
        load.wait()
    resid = tokens_s[...].astype(f32)
    scaled_in = (resid * gain_in_s[...].reshape(1, 64).astype(f32)).astype(bf16)
    square_in = jnp.sum(resid * resid, axis=1, keepdims=True)
    part_q = nn(scaled_in, w_q_s[...])
    part_kv = nn(scaled_in, w_kv_s[...])
    part_rope = nt(scaled_in, w_rope_s[...])
    part_rope = jnp.concatenate([part_rope, jnp.zeros((16, 96), f32)], axis=1)
    part_rope = jnp.where(lane16 == 32, square_in, part_rope)
    groups = [part_q[:, 128 * i : 128 * i + 128] for i in range(4)]
    groups += [part_kv[:, :128], part_kv[:, 128:], part_rope, jnp.zeros((16, 128), f32)]
    for g in range(8):
        for q in range(4):
            part_s[4 * g + q] = groups[g][4 * q : 4 * q + 4]

    for load in loads[5:11]:
        load.wait()
    own_lanes = lane16 // 64 == c
    twice = jnp.concatenate([resid, resid], axis=1)
    pair_small[c, 0:16] = jnp.where(own_lanes, twice, 0.0)
    ao = w_ao_s[0].astype(f32)
    ao = jnp.concatenate([ao, ao], axis=1)
    for i in range(4):
        pair_small[c, 16 + 16 * i : 32 + 16 * i] = jnp.where(own_lanes, ao[16 * i : 16 * i + 16], 0.0)
    gm = gain_mid_s[...].reshape(1, 64).astype(f32)
    gm = jnp.concatenate([gm, gm], axis=1)
    pair_small[c, 80:88] = jnp.where(lane // 64 == c, gm, 0.0)
    pair_big[c, 0:64] = w_in_s[...].astype(f32)
    pair_big[c, 64:128] = w_out_s[...].astype(f32)

    row16 = lax.broadcasted_iota(jnp.int32, (16, 128), 0)
    position = jnp.zeros((16, 128), f32)
    for b in range(SEQS):
        position = jnp.where(row16 == b, lengths_s[b].astype(f32), position)
    angle = position * freq_s[0:1, :]
    low = lax.rem(lane16, 32) < 16
    cos = jnp.cos(angle)
    sin = jnp.sin(angle)
    sin = jnp.where(low, -sin, sin)

    pl.semaphore_wait(barrier, len(z_peers) + len(plane_peers))

    send(part_s.at[2 * t + other], pair_a, 0, partner)
    arrived(pair_a, 0)
    a1[z] = part_s[slot] + pair_a[...]
    for peer in z_peers:
        send(a1.at[z], a1.at[z], 1, peer)
    send(pair_small.at[c], pair_small.at[c], 2, partner)
    send(pair_big.at[c], pair_big.at[c], 3, partner)
    for load in loads[11:]:
        load.wait()
    arrived(a1.at[pl.ds(0, NZ - 1)], 1)
    total = a1[0]
    for i in range(1, NZ):
        total = total + a1[i]
    a2[slot] = total
    for peer in plane_peers:
        send(a2.at[slot], a2.at[slot], 4, peer)
    arrived(a2.at[pl.ds(0, 31)], 4)

    def group(g):
        return jnp.concatenate([a2[4 * g + q] for q in range(4)], axis=0)

    last = group(6)
    raw_q = jnp.concatenate([group(g) for g in range(4)], axis=1)
    raw_kv = jnp.concatenate([group(4), group(5)], axis=1)
    total_in = last[:, 32:33]
    inv_in = lax.rsqrt(total_in / D + EPS)
    mean_q = jnp.sum(raw_q * raw_q, axis=1, keepdims=True) * (1.0 / 512)
    mean_kv = jnp.sum(raw_kv * raw_kv, axis=1, keepdims=True) * (1.0 / 256)
    scale_q = inv_in * lax.rsqrt(inv_in * inv_in * mean_q + EPS)
    scale_kv = inv_in * lax.rsqrt(inv_in * inv_in * mean_kv + EPS)
    query_latent = (raw_q * scale_q * gain_q_s[...].reshape(1, 512).astype(f32)).astype(bf16)
    latent_new = (raw_kv * scale_kv * gain_kv_s[...].reshape(1, 256).astype(f32)).astype(bf16)
    rope_new = rotated(last * inv_in, cos, sin, low).astype(bf16)
    new_latent[...] = latent_new
    new_rope[...] = rope_new[:, :32]
    nl_s[:, 0:256] = latent_new.astype(f32)
    nl_s[:, 256:384] = jnp.where(lane16 < 32, rope_new.astype(f32), 0.0)

    query_nope = nt(query_latent, w_qn_s[...])
    query_rope = nt(query_latent, w_qr_s[...])
    for p in range(8):
        pair = query_nope[:, 128 * p : 128 * p + 128]
        both = jnp.concatenate([jnp.where(lane16 < 64, pair, 0.0), jnp.where(lane16 < 64, 0.0, pair)], axis=0)
        both = nn(both.astype(bf16), w_k_s[128 * p : 128 * p + 128, :])
        both = both.astype(bf16).astype(f32)
        for k in (0, 1):
            qc_s[k, 32 * p : 32 * p + 32, :] = both[:, 128 * k : 128 * k + 128]
    for j in range(4):
        tile = rotated(query_rope[:, 128 * j : 128 * j + 128], cos, sin, low).astype(bf16).astype(f32)
        for i in range(4):
            h = 4 * j + i
            qr_s[16 * h : 16 * h + 16, :] = jnp.where(lane16 // 32 == i, tile, 0.0)

    first = ((2 * z + c) * NT + t) * SPAN
    spot = first + lax.broadcasted_iota(jnp.int32, (16, SPAN), 1)
    scores = []
    for b in range(SEQS):
        qc = jnp.concatenate([qc_s[k, pl.ds(b, 16, stride=16), :] for k in (0, 1)], axis=1).astype(bf16)
        qr = qr_s[pl.ds(b, 16, stride=16), :].astype(bf16)
        keys = rope_s[b]
        keys = jnp.concatenate([keys, keys, keys, keys], axis=0)
        s = (nt(qc, latent_s[b]) + nn(qr, keys)) * SCALE
        scores.append(jnp.where(spot < lengths_s[b], s, -1e30))
    for b in range(SEQS):
        s = scores[b]
        top = jnp.max(s, axis=1, keepdims=True)
        w = jnp.where(spot < lengths_s[b], jnp.exp(s - top), 0.0)
        tot = jnp.sum(w, axis=1, keepdims=True)
        acc = nn(w.astype(bf16), latent_s[b])
        for k in (0, 1):
            acc_s[k, 16 * b : 16 * b + 16, :] = acc[:, 128 * k : 128 * k + 128]
        st_s[16 * b : 16 * b + 16, :] = jnp.where(lane16 == 64, top, jnp.where(lane16 == 65, tot, 0.0))
    for p in range(8):
        wv = w_v_s[128 * p : 128 * p + 128, :]
        rows = [
            jnp.concatenate([acc_s[i, pl.ds(2 * p + k, 16, stride=16), :] for i in (0, 1)], axis=1)
            for k in (0, 1)
        ]
        both = nt(jnp.concatenate(rows, axis=0).astype(bf16), wv)
        for k in (0, 1):
            h = 2 * p + k
            value = both[16 * k : 16 * k + 16]
            if k:
                value = pltpu.roll(value, 64, 1)
            message = jnp.where(lane16 < 64, value, st_s[pl.ds(h, 16, stride=16), :])
            b_send[2 * h] = message[0:8]
            b_send[2 * h + 1] = message[8:16]
    for peer in plane_peers:
        send(b_send.at[2 * peer[2] + peer[1]], b_recv.at[slot], 5, peer)
    b_recv[slot] = b_send[slot]

    rows = pl.ds(pl.multiple_of(8 * c, 8), 8)
    head_rows = pl.ds(pl.multiple_of(16 * t + 8 * c, 8), 8)
    own_latent = nl_s[rows, 0:256]
    own_rope = nl_s[rows, 256:384]
    q_rope = qr_s[head_rows, :]
    q_rope = q_rope + pltpu.roll(q_rope, 64, 1)
    q_rope = q_rope + pltpu.roll(q_rope, 32, 1)
    own_query = jnp.concatenate([qc_s[k, head_rows, :] for k in (0, 1)], axis=1)
    self_score = SCALE * (
        jnp.sum(own_query * own_latent, axis=1, keepdims=True)
        + jnp.sum(q_rope * own_rope, axis=1, keepdims=True)
    )
    own_wv = w_v_s[pl.ds(pl.multiple_of(64 * t, 64), 64), :]
    self_value = nt(own_latent.astype(bf16), own_wv)
    self_value = jnp.concatenate([self_value, jnp.zeros((8, 64), f32)], axis=1)

    arrived(b_recv.at[pl.ds(0, 31)], 5)
    _, message = merged([b_recv[i] for i in range(32)], lane)
    c_recv[z] = message
    for peer in z_peers:
        send(c_recv.at[z], c_recv.at[z], 6, peer)

    arrived(pair_small.at[c], 2)
    arrived(pair_big.at[c], 3)
    w_ao2 = (pair_small[0, 16:80] + pair_small[1, 16:80]).astype(bf16)
    gain2 = pair_small[0, 80:88] + pair_small[1, 80:88]
    resid2 = pair_small[0, rows, :] + pair_small[1, rows, :]
    w_in2 = jnp.concatenate([pair_big[0, 0:64], pair_big[1, 0:64]], axis=0).astype(bf16)
    w_out2 = jnp.concatenate([pair_big[0, 64:128], pair_big[1, 64:128]], axis=0).astype(bf16)

    arrived(c_recv.at[pl.ds(0, NZ - 1)], 6)
    top, message = merged([c_recv[i] for i in range(NZ)], lane)
    joined = jnp.maximum(top, self_score)
    fade = jnp.exp(top - joined)
    self_weight = jnp.exp(self_score - joined)
    total = message[:, 65:66] * fade + self_weight
    values = message * fade + self_weight.astype(bf16).astype(f32) * self_value
    head_out = (values / total)[:, :64].astype(bf16)
    d_recv[t] = nn(head_out, w_ao2)
    for u in t_peers:
        send(d_recv.at[t], d_recv.at[t], 7, (z, c, u))
    arrived(d_recv.at[pl.ds(0, NT - 1)], 7)
    total = d_recv[0]
    for i in range(1, NT):
        total = total + d_recv[i]
    resid_mid = resid2 + total
    rm_all[c] = resid_mid
    send(rm_all.at[c], rm_all.at[c], 8, partner)
    square_mid = jnp.broadcast_to(jnp.sum(resid_mid * resid_mid, axis=1, keepdims=True), (8, 128))
    scaled_mid = (resid_mid * gain2).astype(bf16)
    hidden_part = nn(scaled_mid, w_in2)
    for i in range(4):
        for j in range(4):
            e_send[4 * i + j, 0:2] = hidden_part[2 * i : 2 * i + 2, 128 * j : 128 * j + 128]
            e_send[4 * i + j, 2:4] = square_mid[2 * i : 2 * i + 2]
    for peer in z_peers:
        send(e_send.at[peer[0]], e_recv.at[z], 9, peer)
    e_recv[z] = e_send[z]
    arrived(e_recv.at[pl.ds(0, NZ - 1)], 9)
    total = e_recv[0]
    for i in range(1, NZ):
        total = total + e_recv[i]
    inv_mid = lax.rsqrt(total[2:4] / D + EPS)
    hidden = jnp.square(jnp.maximum(inv_mid * total[0:2], 0.0))
    g_recv[z] = hidden
    for peer in z_peers:
        send(g_recv.at[z], g_recv.at[z], 10, peer)
    arrived(g_recv.at[pl.ds(0, NZ - 1)], 10)
    for i in range(4):
        for j in range(4):
            hid_s[2 * i : 2 * i + 2, 128 * j : 128 * j + 128] = g_recv[4 * i + j]
    f_recv[slot] = nt(hid_s[...].astype(bf16), w_out2)
    for peer in plane_peers:
        send(f_recv.at[slot], f_recv.at[slot], 11, peer)
    arrived(rm_all.at[c], 8)
    arrived(f_recv.at[pl.ds(0, 31)], 11)
    for k in (0, 1):
        total = f_recv[k]
        for i in range(1, NT):
            total = total + f_recv[2 * i + k]
        total = rm_all[k] + total
        total = jnp.where(c == 0, total, pltpu.roll(total, 64, 1))
        mixed[8 * k : 8 * k + 8, :] = total[:, :64].astype(bf16)

    sent(pair_a, 0)
    sent(a1.at[pl.ds(0, NZ - 1)], 1)
    sent(pair_small.at[c], 2)
    sent(pair_big.at[c], 3)
    sent(a2.at[pl.ds(0, 31)], 4)
    sent(b_recv.at[pl.ds(0, 31)], 5)
    sent(c_recv.at[pl.ds(0, NZ - 1)], 6)
    sent(d_recv.at[pl.ds(0, NT - 1)], 7)
    sent(rm_all.at[c], 8)
    sent(e_recv.at[pl.ds(0, NZ - 1)], 9)
    sent(g_recv.at[pl.ds(0, NZ - 1)], 10)
    sent(f_recv.at[pl.ds(0, 31)], 11)


def per_device(tokens, lengths, latent, rope, gain_in, w_q, w_kv, w_rope, gain_q, w_qn, w_qr, gain_kv, w_k, w_v, w_ao, gain_mid, w_in, w_out):
    rope = jnp.swapaxes(rope, 1, 2)
    w_rope = w_rope.T
    w_qn = jnp.transpose(w_qn, (1, 2, 0)).reshape(1024, 512)
    w_qr = jnp.transpose(w_qr, (1, 2, 0)).reshape(512, 512)
    w_k = jnp.transpose(w_k, (1, 2, 0)).reshape(1024, 256)
    w_v = jnp.transpose(w_v, (1, 2, 0)).reshape(1024, 256)
    w_out = w_out.T
    steps = np.arange(128) % 16
    freq = jnp.asarray(np.broadcast_to((10000.0 ** (-steps / 16.0)).astype(np.float32), (8, 128)))
    args = (tokens, lengths, latent, rope, gain_in, w_q, w_kv, w_rope, gain_q, w_qn, w_qr, gain_kv, w_k, w_v, w_ao, gain_mid, w_in, w_out, freq)
    places = [pltpu.SMEM((16,), jnp.int32) if a is lengths else pltpu.VMEM(a.shape, a.dtype) for a in args]
    scratch = [
        pltpu.VMEM((32, 4, 128), f32),
        pltpu.VMEM((4, 128), f32),
        pltpu.VMEM((2, 88, 128), f32),
        pltpu.VMEM((2, 128, 512), f32),
        pltpu.VMEM((NZ, 4, 128), f32),
        pltpu.VMEM((32, 4, 128), f32),
        pltpu.VMEM((2, 256, 128), f32),
        pltpu.VMEM((256, 128), f32),
        pltpu.VMEM((2, 256, 128), f32),
        pltpu.VMEM((256, 128), f32),
        pltpu.VMEM((16, 384), f32),
        pltpu.VMEM((32, 8, 128), f32),
        pltpu.VMEM((32, 8, 128), f32),
        pltpu.VMEM((NZ, 8, 128), f32),
        pltpu.VMEM((NT, 8, 128), f32),
        pltpu.VMEM((2, 8, 128), f32),
        pltpu.VMEM((NZ, 4, 128), f32),
        pltpu.VMEM((NZ, 4, 128), f32),
        pltpu.VMEM((NZ, 2, 128), f32),
        pltpu.VMEM((8, 512), f32),
        pltpu.VMEM((32, 8, 128), f32),
        pltpu.SemaphoreType.DMA((len(args),)),
        pltpu.SemaphoreType.DMA((12,)),
        pltpu.SemaphoreType.DMA((12,)),
    ]
    return pl.pallas_call(
        kernel,
        out_shape=(
            jax.ShapeDtypeStruct((16, 64), bf16),
            jax.ShapeDtypeStruct((16, 256), bf16),
            jax.ShapeDtypeStruct((16, 32), bf16),
        ),
        in_specs=[pl.BlockSpec(memory_space=pl.ANY)] * len(args),
        out_specs=tuple([pl.BlockSpec(memory_space=pltpu.VMEM)] * 3),
        scratch_shapes=places + scratch,
        compiler_params=pltpu.CompilerParams(
            collective_id=0, has_side_effects=True, vmem_limit_bytes=48 * 1024 * 1024
        ),
    )(*args)


def solution(mesh):
    finer = Mesh(mesh.devices.reshape(NZ, 2, NT), ("z", "core", "tp"))
    kv, both, tp = ("z", "core"), ("z", "core", "tp"), "tp"
    in_specs = (
        P(None, kv),
        P(),
        P(None, both, None),
        P(None, both, None),
        P(kv),
        P(kv, None),
        P(kv, None),
        P(kv, None),
        P(),
        P(),
        P(),
        P(),
        P(),
        P(),
        P(tp, None, kv),
        P(kv),
        P(kv, tp),
        P(tp, kv),
    )
    return jax.shard_map(
        per_device, mesh=finer, in_specs=in_specs, out_specs=(P(None, kv), P(), P()), check_vma=False
    )
```
